32 devices in a mesh: fs: 4 (over z), rep: 4 (over y, x), tp: 2 (over core).
Axes of the slice: x: 2, y: 2, z: 4, core: 2. Of those that a mesh axis runs over, the one named last changes fastest.
Arguments:
- saved_input: bfloat16 [5632, 2048], P(('fs', 'rep')), may hold values from -6 to 6
- query_cot: bfloat16 [5632, 1024], P(('fs', 'rep'), 'tp'), may hold values from -0.078125 to 0.078125
- attn_out: bfloat16 [5632, 1024], P(('fs', 'rep'), 'tp'), may hold values from -6 to 6
- out_cot: bfloat16 [5632, 2048], P(('fs', 'rep')), may hold values from -0.078125 to 0.078125
- query_basis: bfloat16 [2048, 512], P('fs'), may hold values from -0.25 to 0.25
- output_basis: bfloat16 [2048, 512], P('fs'), may hold values from -0.25 to 0.25
- query_weight: float32 [2048, 1024], P('fs', 'tp'), may hold values from -6 to 6
- output_weight: float32 [1024, 2048], P('tp', 'fs'), may hold values from -6 to 6
- query_moment: float32 [512, 1024], P('rep', 'tp'), may hold values from -52 to 52
- output_moment: float32 [1024, 512], P('tp', 'rep'), may hold values from -52 to 52
Outputs:
- query_step: float32 [2048, 1024], P('fs', 'tp')
- output_step: float32 [1024, 2048], P('tp', 'fs')
- query_new: float32 [2048, 1024], P('fs', 'tp')
- output_new: float32 [1024, 2048], P('tp', 'fs')
- query_copy: bfloat16 [2048, 1024], P('fs', 'tp')
- output_copy: bfloat16 [1024, 2048], P('tp', 'fs')
- query_moment_new: float32 [512, 1024], P('rep', 'tp')
- output_moment_new: float32 [1024, 512], P('tp', 'rep')
The draws below stay inside these ranges and needn't reach their ends.
All inputs are finite; a program needn't handle non-finite values.
Results may differ from the reference program's by a relative error of at most 0.0029.
Values may be sent and summed in bfloat16 or wider, within the bound.
A program may use at most 64 MiB of HBM per device.

```python
import jax
import jax.numpy as jnp
from jax import lax

D = 2048
HEADS = 16
HEAD_DIM = 64
RANK = 512
HD = 1024
TOKENS = 5632


def scaled_field(key, rows, cols):
    first = jax.random.fold_in(key, 11)
    row_pos = jnp.arange(rows, dtype=jnp.float32) / max(rows - 1, 1)
    col_pos = jnp.arange(cols, dtype=jnp.float32) / max(cols - 1, 1)
    base = jnp.clip(jax.random.normal(first, (rows, cols), jnp.float32), -3.0, 3.0)
    row_scale = 1.0 + 3.0 * row_pos
    col_scale = 1.0 + 2.0 * col_pos
    return base * row_scale[:, None] * col_scale[None, :]


def draw_query_moment(key, part):
    return scaled_field(key, RANK, HEADS * HEAD_DIM)


def draw_output_moment(key, part):
    return scaled_field(jax.random.fold_in(key, 5), HEADS * HEAD_DIM, RANK)


def levels(rng, extent, split, low, high):
    gain, own = 1.0, jax.random.fold_in(rng, 6)
    for axis_at, parts in split:
        steps = jnp.exp(jax.random.uniform(jax.random.fold_in(own, axis_at), (parts,), jnp.float32, low / len(split), high / len(split)))
        gain = gain * jnp.repeat(steps, extent[axis_at] // parts).reshape([-1 if axis == axis_at else 1 for axis in range(len(extent))])
    return gain


def scatter_about(rng, extent, scale, bound, split=(), kind=jnp.bfloat16):
    array = scale * jax.random.normal(rng, extent, jnp.float32)
    if split:
        array = array * levels(rng, extent, split, -0.22, 0.18)
    return jnp.clip(array, -bound, bound).astype(kind)


def setup_inputs(seed: int = 0) -> dict:
    splits = jax.random.split(jax.random.key(seed), 11)
    saved_input = scatter_about(splits[0], (TOKENS, D), 1.0, 6.0, ((0, 16),))
    query_cot = scatter_about(splits[1], (TOKENS, HD), (TOKENS ** -0.5), 0.078125, ((0, 16), (1, 2)))
    attn_out = scatter_about(splits[2], (TOKENS, HD), 1.0, 6.0, ((0, 16), (1, 2)))
    out_cot = scatter_about(splits[3], (TOKENS, D), (TOKENS ** -0.5), 0.078125, ((0, 16),))
    query_basis = scatter_about(splits[4], (D, RANK), RANK ** -0.5, 0.25, ((0, 4),))
    output_basis = scatter_about(splits[5], (D, RANK), RANK ** -0.5, 0.25, ((0, 4),))
    query_weight = scatter_about(splits[6], (D, HD), 1.0, 6.0, ((0, 4), (1, 2)), jnp.float32)
    output_weight = scatter_about(splits[7], (HD, D), 1.0, 6.0, ((0, 2), (1, 4)), jnp.float32)
    query_moment = draw_query_moment(jax.random.fold_in(splits[10], 71), 0)
    output_moment = draw_output_moment(jax.random.fold_in(splits[10], 71), 0)
    return dict(saved_input=saved_input, query_cot=query_cot, attn_out=attn_out, out_cot=out_cot, query_basis=query_basis, output_basis=output_basis, query_weight=query_weight, output_weight=output_weight, query_moment=query_moment, output_moment=output_moment)


BETA = 0.8
RATE = 0.2
EPS = 1e-06

def normalize(moment):
    scale = lax.rsqrt(jnp.mean(moment * moment) + EPS)
    return (moment * scale).astype(jnp.bfloat16)

def reference(saved_input, query_cot, attn_out, out_cot, query_basis, output_basis, query_weight, output_weight, query_moment, output_moment):
    query_grad = jnp.dot(saved_input.T, query_cot, preferred_element_type=jnp.float32)
    query_proj = jnp.dot(query_basis.astype(jnp.float32).T, query_grad, precision=lax.Precision.HIGHEST)
    cot_proj = jnp.dot(out_cot, output_basis, preferred_element_type=jnp.float32)
    output_proj = jnp.dot(attn_out.astype(jnp.float32).T, cot_proj, precision=lax.Precision.HIGHEST)
    query_moment_new = BETA * query_moment + (1.0 - BETA) * query_proj
    output_moment_new = BETA * output_moment + (1.0 - BETA) * output_proj
    query_dir = normalize(query_moment_new)
    output_dir = normalize(output_moment_new)
    query_step = jnp.dot(query_basis, query_dir, preferred_element_type=jnp.float32)
    output_step = jnp.dot(output_dir, output_basis.T, preferred_element_type=jnp.float32)
    query_new = query_weight - RATE * query_step
    output_new = output_weight - RATE * output_step
    return (query_step, output_step, query_new, output_new, query_new.astype(jnp.bfloat16), output_new.astype(jnp.bfloat16), query_moment_new, output_moment_new)
```

```python
import functools

import jax
import jax.numpy as jnp
from jax import lax
from jax.experimental import pallas as pl
from jax.experimental.pallas import tpu as pltpu
from jax.sharding import PartitionSpec as P

BETA = 0.8
RATE = 0.2
EPS = 1e-06


def on_device(
    saved_input,
    query_cot,
    attn_out,
    out_cot,
    query_basis,
    output_basis,
    query_weight,
    output_weight,
    query_moment,
    output_moment,
):
    rank = query_basis.shape[1]
    grad_rows = lax.psum_scatter(
        jnp.dot(saved_input.T, query_cot, preferred_element_type=jnp.float32),
        "fs",
        scatter_dimension=0,
        tiled=True,
    )
    query_part = jnp.dot(
        query_basis.astype(jnp.float32).T, grad_rows, precision=lax.Precision.HIGHEST
    )
    cot_proj = jnp.dot(
        out_cot,
        lax.all_gather(output_basis, "fs", axis=0, tiled=True),
        preferred_element_type=jnp.float32,
    )
    output_part = jnp.dot(attn_out.astype(jnp.float32).T, cot_proj, precision=lax.Precision.HIGHEST)
    reps = lax.axis_size("rep")
    share = rank // reps
    query_terms, output_terms = (
        lax.all_to_all(
            query_part.astype(jnp.bfloat16), "rep", split_axis=0, concat_axis=0, tiled=True
        ).astype(query_part.dtype),
        lax.all_to_all(
            output_part.T.astype(jnp.bfloat16), "rep", split_axis=0, concat_axis=0, tiled=True
        ).astype(jnp.float32),
    )
    width = query_part.shape[1]
    query_local = jnp.sum(query_terms.reshape(reps, share, width), axis=0)
    output_local = jnp.sum(output_terms.reshape(reps, share, width), axis=0)
    query_share, output_flip = lax.psum((query_local, output_local), "fs")
    output_share = output_flip.T
    query_moment_new = BETA * query_moment + (1.0 - BETA) * query_share
    output_moment_new = BETA * output_moment + (1.0 - BETA) * output_share
    query_squares, output_squares = lax.psum(
        (
            jnp.sum(query_moment_new * query_moment_new),
            jnp.sum(output_moment_new * output_moment_new),
        ),
        ("rep", "tp"),
    )
    entries = rank * query_moment.shape[1] * lax.axis_size("tp")
    query_dir = (query_moment_new * lax.rsqrt(query_squares / entries + EPS)).astype(jnp.bfloat16)
    output_dir = (output_moment_new * lax.rsqrt(output_squares / entries + EPS)).astype(
        jnp.bfloat16
    )
    query_full, output_full = (
        lax.all_gather(query_dir, "rep", axis=0, tiled=True),
        lax.all_gather(output_dir, "rep", axis=1, tiled=True),
    )
    query_step = jnp.dot(query_basis, query_full, preferred_element_type=jnp.float32)
    output_step = jnp.dot(output_full, output_basis.T, preferred_element_type=jnp.float32)
    query_new = query_weight - RATE * query_step
    output_new = output_weight - RATE * output_step
    return (
        query_step,
        output_step,
        query_new,
        output_new,
        query_new.astype(jnp.bfloat16),
        output_new.astype(jnp.bfloat16),
        query_moment_new,
        output_moment_new,
    )


MESH = pl.DeviceIdType.MESH


def exchange_kernel(
    entries,
    si_hbm, oc_hbm, qc_hbm, ao_hbm, qb_hbm, ob_hbm, mq_hbm, mo_hbm,
    full_out, mom_out,
    act, cot, base, mq, mo, gath, xb, pb, t1, t2, mom, nrm, full,
    load_sem, store_sem, az_s, az_r, aw_s, aw_r, xc_s, xc_r,
    b1_s, b1_r, b2_s, b2_r, n_s, n_r, d_s, d_r,
):
    f, r, t = lax.axis_index("fs"), lax.axis_index("rep"), lax.axis_index("tp")
    y, x = r // 2, r % 2
    ot = 1 - t
    fpeer = [(f + d) % 4 for d in (1, 3, 2)]
    fsrc = [(f + 4 - d) % 4 for d in (1, 3, 2)]
    rpeer = [2 * y + (1 - x), 2 * (1 - y) + x, 3 - r]
    depth, rank = base.shape[1], base.shape[2]
    hd, hr = depth // 2, rank // 2
    share = rank // 4

    loads = []
    for k, (src, dst) in enumerate((
        (qb_hbm, base.at[0]), (ob_hbm, base.at[1]), (si_hbm, act.at[0]), (oc_hbm, act.at[1]),
        (qc_hbm, cot.at[0]), (ao_hbm, cot.at[1]), (mq_hbm, mq), (mo_hbm, mo),
    )):
        c = pltpu.make_async_copy(src, dst, load_sem.at[k])
        c.start()
        loads.append(c)

    barrier = pltpu.get_barrier_semaphore()
    for g in fpeer:
        pl.semaphore_signal(barrier, inc=1, device_id=(g, r, t), device_id_type=MESH)
    for q in rpeer:
        for s in (t, ot):
            pl.semaphore_signal(barrier, inc=1, device_id=(f, q, s), device_id_type=MESH)
    pl.semaphore_signal(barrier, inc=1, device_id=(f, r, ot), device_id_type=MESH)
    pl.semaphore_wait(barrier, 10)

    def remote(src, dst, ss, rs, dev):
        return pltpu.make_async_remote_copy(
            src_ref=src, dst_ref=dst, send_sem=ss, recv_sem=rs, device_id=dev, device_id_type=MESH
        )

    half = (x, y)
    near = (rpeer[0], rpeer[1])
    cols = pl.ds(pl.multiple_of(t * hr, hr), hr)
    sends = []
    zs = [[], []]
    for p in range(2):
        loads[p].wait()
        rows = pl.ds(pl.multiple_of(half[p] * hd, hd), hd)
        for k in range(3):
            c = remote(
                base.at[p, rows, cols], gath.at[p, f, rows, :],
                az_s.at[p, k], az_r.at[p, k], (fpeer[k], r, t),
            )
            c.start()
            zs[p].append(c)
    ws = [[], []]
    for k in range(3):
        for p in range(2):
            rows = pl.ds(pl.multiple_of(half[p] * hd, hd), hd)
            zs[p][k].wait_recv()
            c = remote(
                gath.at[p, fsrc[k], rows, :], gath.at[p, fsrc[k], rows, :],
                aw_s.at[p, k], aw_r.at[p, k], (f, near[p], t),
            )
            c.start()
            ws[p].append(c)

    def slab(p, g, weights):
        return jnp.dot(
            act[p, :, pl.ds(pl.multiple_of(g * depth, depth), depth)], weights,
            preferred_element_type=jnp.float32,
        )

    loads[2].wait()
    loads[3].wait()
    accs = [slab(p, f, base[p, :, cols]) for p in range(2)]
    xs = []
    for p in range(2):
        acc = accs[p]
        for k in range(3):
            ws[p][k].wait_recv()
            acc = acc + slab(p, fsrc[k], gath[p, fsrc[k]])
        xb[p, t] = acc.astype(jnp.bfloat16)
        c = remote(xb.at[p, t], xb.at[p, t], xc_s.at[p], xc_r.at[p], (f, r, ot))
        c.start()
        xs.append(c)

    b1 = [[], []]
    for p in range(2):
        loads[4 + p].wait()
        xs[p].wait_recv()
        for j in range(2):
            part = lax.dot_general(
                xb[p, j], cot[p], (((0,), (0,)), ((), ())), preferred_element_type=jnp.float32
            )
            for i in range(2):
                pb[p, 2 * j + i] = part[i * share : (i + 1) * share].astype(jnp.bfloat16)
        for k in (2, 0, 1):
            c = remote(
                pb.at[p, rpeer[k]], t1.at[p, k], b1_s.at[p, k], b1_r.at[p, k], (f, rpeer[k], t)
            )
            c.start()
            b1[p].append(c)

    b2 = [[], []]
    for p in range(2):
        for c in b1[p]:
            c.wait_recv()
        total = pb[p, r].astype(jnp.float32)
        for k in range(3):
            total = total + t1[p, k].astype(jnp.float32)
        t2[p, f] = total.astype(jnp.bfloat16)
        for k in (2, 0, 1):
            c = remote(
                t2.at[p, f], t2.at[p, f], b2_s.at[p, k], b2_r.at[p, k], (fpeer[k], r, t)
            )
            c.start()
            b2[p].append(c)

    loads[6].wait()
    loads[7].wait()
    others = [(q, s) for q in rpeer for s in (t, ot)] + [(r, ot)]
    ns = [[], []]
    me = 2 * r + t
    for p in range(2):
        old = mq[...] if p == 0 else mo[...].T
        for c in b2[p]:
            c.wait_recv()
        total = t2[p, 0].astype(jnp.float32)
        for g in range(1, 4):
            total = total + t2[p, g].astype(jnp.float32)
        new = BETA * old + (1.0 - BETA) * total
        mom[p] = new
        sq = new * new
        lanes = sq[:, :128]
        for k in range(1, sq.shape[1] // 128):
            lanes = lanes + sq[:, k * 128 : (k + 1) * 128]
        acc = lanes[:8]
        for k in range(1, share // 8):
            acc = acc + lanes[k * 8 : (k + 1) * 8]
        nrm[p, me] = acc
        for k, (q, s) in enumerate(others):
            c = remote(nrm.at[p, me], nrm.at[p, me], n_s.at[p, k], n_r.at[p, k], (f, q, s))
            c.start()
            ns[p].append(c)

    stores = []
    ds = [[], []]
    for p in range(2):
        c = pltpu.make_async_copy(mom.at[p], mom_out.at[p], store_sem.at[p])
        c.start()
        stores.append(c)
        for c in ns[p]:
            c.wait_recv()
        acc = nrm[p, 0]
        for k in range(1, 8):
            acc = acc + nrm[p, k]
        squares = jnp.sum(jnp.sum(acc, axis=0, keepdims=True), axis=1, keepdims=True)
        full[p, r] = (mom[p] * lax.rsqrt(squares / entries + EPS)).astype(jnp.bfloat16)
        for k in (2, 0, 1):
            c = remote(
                full.at[p, r], full.at[p, r], d_s.at[p, k], d_r.at[p, k], (f, rpeer[k], t)
            )
            c.start()
            ds[p].append(c)
    for p in range(2):
        for c in ds[p]:
            c.wait_recv()
        c = pltpu.make_async_copy(full.at[p], full_out.at[p], store_sem.at[2 + p])
        c.start()
        stores.append(c)
    for group in (zs, ws, b1, b2, ns, ds, [xs]):
        for part in group:
            for c in part:
                c.wait_send()
    for c in stores:
        c.wait()


def finish_kernel(
    qb, ob, fq, fo, qw, ow, mq, mo, qs_o, os_o, qn_o, on_o, qc_o, oc_o, mq_o, mo_o
):
    step = jnp.dot(qb[...], fq[0], preferred_element_type=jnp.float32)
    new = qw[...] - RATE * step
    qs_o[...] = step
    qn_o[...] = new
    qc_o[...] = new.astype(jnp.bfloat16)
    step = lax.dot_general(
        fo[0].T, ob[...], (((1,), (1,)), ((), ())), preferred_element_type=jnp.float32
    )
    new = ow[...] - RATE * step
    os_o[...] = step
    on_o[...] = new
    oc_o[...] = new.astype(jnp.bfloat16)
    mq_o[...] = mq[0]
    mo_o[...] = mo[0].T


def on_device_fast(
    saved_input, query_cot, attn_out, out_cot, query_basis, output_basis,
    query_weight, output_weight, query_moment, output_moment,
):
    tokens, depth_all = saved_input.shape
    width = query_cot.shape[1]
    depth, rank = query_basis.shape
    share = rank // 4
    entries = rank * width * lax.axis_size("tp")
    bf, f32 = jnp.bfloat16, jnp.float32
    any_spec = pl.BlockSpec(memory_space=pl.ANY)
    dma = pltpu.SemaphoreType.DMA
    full, mom = pl.pallas_call(
        functools.partial(exchange_kernel, entries),
        out_shape=(
            jax.ShapeDtypeStruct((2, 4, share, width), bf),
            jax.ShapeDtypeStruct((2, share, width), f32),
        ),
        in_specs=[any_spec] * 8,
        out_specs=(any_spec, any_spec),
        scratch_shapes=[
            pltpu.VMEM((2, tokens, depth_all), bf),
            pltpu.VMEM((2, tokens, width), bf),
            pltpu.VMEM((2, depth, rank), bf),
            pltpu.VMEM((share, width), f32),
            pltpu.VMEM((width, share), f32),
            pltpu.VMEM((2, 4, depth, rank // 2), bf),
            pltpu.VMEM((2, 2, tokens, rank // 2), bf),
            pltpu.VMEM((2, 4, share, width), bf),
            pltpu.VMEM((2, 3, share, width), bf),
            pltpu.VMEM((2, 4, share, width), bf),
            pltpu.VMEM((2, share, width), f32),
            pltpu.VMEM((2, 8, 8, 128), f32),
            pltpu.VMEM((2, 4, share, width), bf),
            dma((8,)), dma((4,)),
            dma((2, 3)), dma((2, 3)), dma((2, 3)), dma((2, 3)),
            dma((2,)), dma((2,)),
            dma((2, 3)), dma((2, 3)), dma((2, 3)), dma((2, 3)),
            dma((2, 7)), dma((2, 7)), dma((2, 3)), dma((2, 3)),
        ],
        compiler_params=pltpu.CompilerParams(
            collective_id=0, has_side_effects=True, vmem_limit_bytes=60 * 2**20
        ),
    )(
        saved_input, out_cot, query_cot, attn_out, query_basis, output_basis,
        query_moment, output_moment,
    )
    full = full.reshape(2, rank, width)
    n = 4
    rows = pl.BlockSpec((depth // n, rank), lambda i: (i, 0))
    whole = pl.BlockSpec((depth, rank), lambda i: (0, 0))
    wq = pl.BlockSpec((depth // n, width), lambda i: (i, 0))
    wo = pl.BlockSpec((width // n, depth), lambda i: (i, 0))
    mq = pl.BlockSpec((share // n, width), lambda i: (i, 0))
    mo = pl.BlockSpec((width // n, share), lambda i: (i, 0))
    sq, so = query_weight.shape, output_weight.shape
    return pl.pallas_call(
        finish_kernel,
        grid=(n,),
        out_shape=tuple(
            jax.ShapeDtypeStruct(s, d)
            for s, d in (
                (sq, f32), (so, f32), (sq, f32), (so, f32), (sq, bf), (so, bf),
                (query_moment.shape, f32), (output_moment.shape, f32),
            )
        ),
        in_specs=[
            rows, whole,
            pl.BlockSpec((1, rank, width), lambda i: (0, 0, 0)),
            pl.BlockSpec((1, rank, width // n), lambda i: (1, 0, i)),
            wq, wo,
            pl.BlockSpec((1, share // n, width), lambda i: (0, i, 0)),
            pl.BlockSpec((1, share, width // n), lambda i: (1, 0, i)),
        ],
        out_specs=(wq, wo, wq, wo, wq, wo, mq, mo),
        cost_estimate=pl.CostEstimate(
            flops=4 * depth * rank * width, bytes_accessed=20 * depth * width, transcendentals=0
        ),
    )(query_basis, output_basis, full, full, query_weight, output_weight, mom, mom)


def solution(mesh):
    small = dict(mesh.shape) == {"fs": 4, "rep": 4, "tp": 2}
    body = on_device_fast if small else on_device
    placed = (
        P(("fs", "rep"), None),
        P(("fs", "rep"), "tp"),
        P(("fs", "rep"), "tp"),
        P(("fs", "rep"), None),
        P("fs", None),
        P("fs", None),
        P("fs", "tp"),
        P("tp", "fs"),
        P("rep", "tp"),
        P("tp", "rep"),
    )
    return jax.shard_map(
        body,
        mesh=mesh,
        in_specs=placed,
        out_specs=(
            P("fs", "tp"),
            P("tp", "fs"),
            P("fs", "tp"),
            P("tp", "fs"),
            P("fs", "tp"),
            P("tp", "fs"),
            P("rep", "tp"),
            P("tp", "rep"),
        ),
        check_vma=False,
    )
```

```python
import functools

import jax
import jax.numpy as jnp
from jax import lax
from jax.experimental import pallas as pl
from jax.experimental.pallas import tpu as pltpu
from jax.sharding import PartitionSpec as P

BETA = 0.8
RATE = 0.2
EPS = 1e-06


def on_device(
    saved_input,
    query_cot,
    attn_out,
    out_cot,
    query_basis,
    output_basis,
    query_weight,
    output_weight,
    query_moment,
    output_moment,
):
    rank = query_basis.shape[1]
    grad_rows = lax.psum_scatter(
        jnp.dot(saved_input.T, query_cot, preferred_element_type=jnp.float32),
        "fs",
        scatter_dimension=0,
        tiled=True,
    )
    query_part = jnp.dot(
        query_basis.astype(jnp.float32).T, grad_rows, precision=lax.Precision.HIGHEST
    )
    cot_proj = jnp.dot(
        out_cot,
        lax.all_gather(output_basis, "fs", axis=0, tiled=True),
        preferred_element_type=jnp.float32,
    )
    output_part = jnp.dot(attn_out.astype(jnp.float32).T, cot_proj, precision=lax.Precision.HIGHEST)
    reps = lax.axis_size("rep")
    share = rank // reps
    query_terms, output_terms = (
        lax.all_to_all(
            query_part.astype(jnp.bfloat16), "rep", split_axis=0, concat_axis=0, tiled=True
        ).astype(query_part.dtype),
        lax.all_to_all(
            output_part.T.astype(jnp.bfloat16), "rep", split_axis=0, concat_axis=0, tiled=True
        ).astype(jnp.float32),
    )
    width = query_part.shape[1]
    query_local = jnp.sum(query_terms.reshape(reps, share, width), axis=0)
    output_local = jnp.sum(output_terms.reshape(reps, share, width), axis=0)
    query_share, output_flip = lax.psum((query_local, output_local), "fs")
    output_share = output_flip.T
    query_moment_new = BETA * query_moment + (1.0 - BETA) * query_share
    output_moment_new = BETA * output_moment + (1.0 - BETA) * output_share
    query_squares, output_squares = lax.psum(
        (
            jnp.sum(query_moment_new * query_moment_new),
            jnp.sum(output_moment_new * output_moment_new),
        ),
        ("rep", "tp"),
    )
    entries = rank * query_moment.shape[1] * lax.axis_size("tp")
    query_dir = (query_moment_new * lax.rsqrt(query_squares / entries + EPS)).astype(jnp.bfloat16)
    output_dir = (output_moment_new * lax.rsqrt(output_squares / entries + EPS)).astype(
        jnp.bfloat16
    )
    query_full, output_full = (
        lax.all_gather(query_dir, "rep", axis=0, tiled=True),
        lax.all_gather(output_dir, "rep", axis=1, tiled=True),
    )
    query_step = jnp.dot(query_basis, query_full, preferred_element_type=jnp.float32)
    output_step = jnp.dot(output_full, output_basis.T, preferred_element_type=jnp.float32)
    query_new = query_weight - RATE * query_step
    output_new = output_weight - RATE * output_step
    return (
        query_step,
        output_step,
        query_new,
        output_new,
        query_new.astype(jnp.bfloat16),
        output_new.astype(jnp.bfloat16),
        query_moment_new,
        output_moment_new,
    )


MESH = pl.DeviceIdType.MESH


def exchange_kernel(
    entries,
    si_hbm, oc_hbm, qc_hbm, ao_hbm, qb_hbm, ob_hbm, mq_hbm, mo_hbm,
    full_out, mom_out,
    act, cot, base, mq, mo, gath, xb, pb, t1, sb, t2, ag, mom, nrm, full,
    load_sem, store_sem, az_s, az_r, aw_s, aw_r, xc_s, xc_r,
    b1_s, b1_r, b2_s, b2_r, g_s, g_r, n_s, n_r, d_s, d_r,
):
    f, r, t = lax.axis_index("fs"), lax.axis_index("rep"), lax.axis_index("tp")
    y, x = r // 2, r % 2
    ot = 1 - t
    fpeer = [(f + d) % 4 for d in (1, 3, 2)]
    fsrc = [(f + 4 - d) % 4 for d in (1, 3, 2)]
    rpeer = [2 * y + (1 - x), 2 * (1 - y) + x, 3 - r]
    depth, rank = base.shape[1], base.shape[2]
    hd, hr = depth // 2, rank // 2
    share = rank // 4

    loads = []
    for k, (src, dst) in enumerate((
        (qb_hbm, base.at[0]), (ob_hbm, base.at[1]), (si_hbm, act.at[0]), (oc_hbm, act.at[1]),
        (qc_hbm, cot.at[0]), (ao_hbm, cot.at[1]), (mq_hbm, mq), (mo_hbm, mo),
    )):
        c = pltpu.make_async_copy(src, dst, load_sem.at[k])
        c.start()
        loads.append(c)

    barrier = pltpu.get_barrier_semaphore()
    for g in fpeer:
        pl.semaphore_signal(barrier, inc=1, device_id=(g, r, t), device_id_type=MESH)
    for q in rpeer:
        for s in (t, ot):
            pl.semaphore_signal(barrier, inc=1, device_id=(f, q, s), device_id_type=MESH)
    pl.semaphore_signal(barrier, inc=1, device_id=(f, r, ot), device_id_type=MESH)
    pl.semaphore_wait(barrier, 10)

    def remote(src, dst, ss, rs, dev):
        return pltpu.make_async_remote_copy(
            src_ref=src, dst_ref=dst, send_sem=ss, recv_sem=rs, device_id=dev, device_id_type=MESH
        )

    h = x * (1 - t) + y * t
    near = rpeer[0] * (1 - t) + rpeer[1] * t
    rows = pl.ds(pl.multiple_of(h * hd, hd), hd)
    cols = pl.ds(pl.multiple_of(t * hr, hr), hr)
    last = 3

    def line(p, way, s, arrive=False):
        step = -1 if way == 0 else 1
        slab = f + step * s + (step if arrive else 0)
        dst = gath.at[p, slab, rows, :]
        src = base.at[p, rows, cols] if s == 0 and not arrive else dst
        dev = f + step if arrive else f - step
        return remote(src, dst, az_s.at[p, way, s], az_r.at[p, way, s], (dev, r, t))

    def sends_line(way, s):
        return (f >= s) & (f < last) if way == 0 else (f + s <= last) & (f > 0)

    def gets_line(way, s):
        return f >= s + 1 if way == 0 else f + s + 1 <= last

    def share_slab(p, slab):
        return remote(
            gath.at[p, slab, rows, :], gath.at[p, slab, rows, :],
            aw_s.at[p, slab], aw_r.at[p, slab], (f, near, t),
        )

    def got_slab(p, slab):
        orow = pl.ds(pl.multiple_of((1 - h) * hd, hd), hd)
        return remote(
            gath.at[p, slab, orow, :], gath.at[p, slab, orow, :],
            aw_s.at[p, slab], aw_r.at[p, slab], (f, near, t),
        )

    def open_line(p):
        loads[p].wait()
        for way in range(2):
            @pl.when(sends_line(way, 0))
            def _():
                line(p, way, 0).start()

    def run_line(s, p):
        for way in range(2):
            @pl.when(gets_line(way, s))
            def _():
                line(p, way, s, True).wait_recv()
                slab = f - 1 - s if way == 0 else f + 1 + s
                share_slab(p, slab).start()
            if s < 2:
                @pl.when(sends_line(way, s + 1))
                def _():
                    line(p, way, s + 1).start()

    def slab_dot(p, g, weights):
        return jnp.dot(
            act[p, :, pl.ds(pl.multiple_of(g * depth, depth), depth)], weights,
            preferred_element_type=jnp.float32,
        )

    def project(p, acc):
        for g in fsrc:
            got_slab(p, g).wait_recv()
            acc = acc + slab_dot(p, g, gath[p, g])
        xb[p, t] = acc.astype(jnp.bfloat16)
        c = remote(xb.at[p, t], xb.at[p, t], xc_s.at[p], xc_r.at[p], (f, r, ot))
        c.start()
        return c

    def got_half(p):
        return remote(xb.at[p, ot], xb.at[p, ot], xc_s.at[p], xc_r.at[p], (f, r, ot))

    def scatter_reps(p):
        loads[4 + p].wait()
        got_half(p).wait_recv()
        for j in range(2):
            part = lax.dot_general(
                xb[p, j], cot[p], (((0,), (0,)), ((), ())), preferred_element_type=jnp.float32
            )
            for i in range(2):
                pb[p, 2 * j + i] = part[i * share : (i + 1) * share].astype(jnp.bfloat16)
        out = []
        for k in (2, 0, 1):
            c = remote(
                pb.at[p, rpeer[k]], t1.at[p, k], b1_s.at[p, k], b1_r.at[p, k], (f, rpeer[k], t)
            )
            c.start()
            out.append(c)
        return out

    piece = share // 4

    def scatter_tokens(p, arrivals):
        for c in arrivals:
            c.wait_recv()
        total = pb[p, r].astype(jnp.float32)
        for k in range(3):
            total = total + t1[p, k].astype(jnp.float32)
        for g in range(4):
            sb[p, g] = total[g * piece : (g + 1) * piece].astype(jnp.bfloat16)
        out = []
        for k in (2, 0, 1):
            c = remote(
                sb.at[p, fpeer[k]], t2.at[p, k], b2_s.at[p, k], b2_r.at[p, k], (fpeer[k], r, t)
            )
            c.start()
            out.append(c)
        return out

    def gather_sums(p, arrivals):
        for c in arrivals:
            c.wait_recv()
        total = sb[p, f].astype(jnp.float32)
        for k in range(3):
            total = total + t2[p, k].astype(jnp.float32)
        ag[p, f] = total.astype(jnp.bfloat16)
        out = []
        for k in (2, 0, 1):
            c = remote(
                ag.at[p, f], ag.at[p, f], g_s.at[p, k], g_r.at[p, k], (fpeer[k], r, t)
            )
            c.start()
            out.append(c)
        return out

    def got_sums(p, k):
        src = fsrc[k]
        return remote(ag.at[p, src], ag.at[p, src], g_s.at[p, k], g_r.at[p, k], (src, r, t))

    others = [(q, s) for q in rpeer for s in (t, ot)] + [(r, ot)]
    me = 2 * r + t

    def update_moment(p):
        old = mq[...] if p == 0 else mo[...].T
        for k in range(3):
            got_sums(p, k).wait_recv()
        total = ag[p].astype(jnp.float32).reshape(old.shape)
        new = BETA * old + (1.0 - BETA) * total
        mom[p] = new
        sq = new * new
        lanes = sq[:, :128]
        for k in range(1, sq.shape[1] // 128):
            lanes = lanes + sq[:, k * 128 : (k + 1) * 128]
        acc = lanes[:8]
        for k in range(1, share // 8):
            acc = acc + lanes[k * 8 : (k + 1) * 8]
        nrm[p, me] = acc
        out = []
        for k, (q, s) in enumerate(others):
            c = remote(nrm.at[p, me], nrm.at[p, me], n_s.at[p, k], n_r.at[p, k], (f, q, s))
            c.start()
            out.append(c)
        return out

    def gather_dirs(p):
        for k, (q, s) in enumerate(others):
            slot = 2 * q + s
            remote(
                nrm.at[p, slot], nrm.at[p, slot], n_s.at[p, k], n_r.at[p, k], (f, q, s)
            ).wait_recv()
        acc = nrm[p, 0]
        for k in range(1, 8):
            acc = acc + nrm[p, k]
        squares = jnp.sum(jnp.sum(acc, axis=0, keepdims=True), axis=1, keepdims=True)
        full[p, r] = (mom[p] * lax.rsqrt(squares / entries + EPS)).astype(jnp.bfloat16)
        out = []
        for k in (2, 0, 1):
            c = remote(
                full.at[p, r], full.at[p, r], d_s.at[p, k], d_r.at[p, k], (f, rpeer[k], t)
            )
            c.start()
            out.append(c)
        return out

    open_line(0)
    open_line(1)
    loads[2].wait()
    loads[3].wait()
    accs = [slab_dot(p, f, base[p, :, cols]) for p in range(2)]
    for s in range(3):
        run_line(s, 0)
        run_line(s, 1)
    x0 = project(0, accs[0])
    b1q = scatter_reps(0)
    x1 = project(1, accs[1])
    b2q = scatter_tokens(0, b1q)
    b1o = scatter_reps(1)
    gq = gather_sums(0, b2q)
    b2o = scatter_tokens(1, b1o)
    loads[6].wait()
    nq = update_moment(0)
    go = gather_sums(1, b2o)
    dq = gather_dirs(0)
    loads[7].wait()
    no = update_moment(1)
    stores = []
    for p in range(2):
        c = pltpu.make_async_copy(mom.at[p], mom_out.at[p], store_sem.at[p])
        c.start()
        stores.append(c)
    do = gather_dirs(1)
    for p in range(2):
        for k in range(3):
            remote(
                full.at[p, rpeer[k]], full.at[p, rpeer[k]],
                d_s.at[p, k], d_r.at[p, k], (f, rpeer[k], t),
            ).wait_recv()
        c = pltpu.make_async_copy(full.at[p], full_out.at[p], store_sem.at[2 + p])
        c.start()
        stores.append(c)
    for p in range(2):
        for s in range(3):
            for way in range(2):
                @pl.when(sends_line(way, s))
                def _():
                    line(p, way, s).wait_send()
        for g in fsrc:
            share_slab(p, g).wait_send()
    for group in (b1q, b1o, b2q, b2o, gq, go, nq, no, dq, do, [x0, x1]):
        for c in group:
            c.wait_send()
    for c in stores:
        c.wait()


def finish_kernel(
    qb, ob, fq, fo, qw, ow, mq, mo, qs_o, os_o, qn_o, on_o, qc_o, oc_o, mq_o, mo_o
):
    step = jnp.dot(qb[...], fq[0], preferred_element_type=jnp.float32)
    new = qw[...] - RATE * step
    qs_o[...] = step
    qn_o[...] = new
    qc_o[...] = new.astype(jnp.bfloat16)
    step = lax.dot_general(
        fo[0].T, ob[...], (((1,), (1,)), ((), ())), preferred_element_type=jnp.float32
    )
    new = ow[...] - RATE * step
    os_o[...] = step
    on_o[...] = new
    oc_o[...] = new.astype(jnp.bfloat16)
    mq_o[...] = mq[0]
    mo_o[...] = mo[0].T


def on_device_fast(
    saved_input, query_cot, attn_out, out_cot, query_basis, output_basis,
    query_weight, output_weight, query_moment, output_moment,
):
    tokens, depth_all = saved_input.shape
    width = query_cot.shape[1]
    depth, rank = query_basis.shape
    share = rank // 4
    entries = rank * width * lax.axis_size("tp")
    bf, f32 = jnp.bfloat16, jnp.float32
    any_spec = pl.BlockSpec(memory_space=pl.ANY)
    dma = pltpu.SemaphoreType.DMA
    full, mom = pl.pallas_call(
        functools.partial(exchange_kernel, entries),
        out_shape=(
            jax.ShapeDtypeStruct((2, 4, share, width), bf),
            jax.ShapeDtypeStruct((2, share, width), f32),
        ),
        in_specs=[any_spec] * 8,
        out_specs=(any_spec, any_spec),
        scratch_shapes=[
            pltpu.VMEM((2, tokens, depth_all), bf),
            pltpu.VMEM((2, tokens, width), bf),
            pltpu.VMEM((2, depth, rank), bf),
            pltpu.VMEM((share, width), f32),
            pltpu.VMEM((width, share), f32),
            pltpu.VMEM((2, 4, depth, rank // 2), bf),
            pltpu.VMEM((2, 2, tokens, rank // 2), bf),
            pltpu.VMEM((2, 4, share, width), bf),
            pltpu.VMEM((2, 3, share, width), bf),
            pltpu.VMEM((2, 4, share // 4, width), bf),
            pltpu.VMEM((2, 3, share // 4, width), bf),
            pltpu.VMEM((2, 4, share // 4, width), bf),
            pltpu.VMEM((2, share, width), f32),
            pltpu.VMEM((2, 8, 8, 128), f32),
            pltpu.VMEM((2, 4, share, width), bf),
            dma((8,)), dma((4,)),
            dma((2, 2, 3)), dma((2, 2, 3)), dma((2, 4)), dma((2, 4)),
            dma((2,)), dma((2,)),
            dma((2, 3)), dma((2, 3)), dma((2, 3)), dma((2, 3)), dma((2, 3)), dma((2, 3)),
            dma((2, 7)), dma((2, 7)), dma((2, 3)), dma((2, 3)),
        ],
        compiler_params=pltpu.CompilerParams(
            collective_id=0, has_side_effects=True, vmem_limit_bytes=60 * 2**20
        ),
    )(
        saved_input, out_cot, query_cot, attn_out, query_basis, output_basis,
        query_moment, output_moment,
    )
    full = full.reshape(2, rank, width)
    n = 4
    rows = pl.BlockSpec((depth // n, rank), lambda i: (i, 0))
    whole = pl.BlockSpec((depth, rank), lambda i: (0, 0))
    wq = pl.BlockSpec((depth // n, width), lambda i: (i, 0))
    wo = pl.BlockSpec((width // n, depth), lambda i: (i, 0))
    mq = pl.BlockSpec((share // n, width), lambda i: (i, 0))
    mo = pl.BlockSpec((width // n, share), lambda i: (i, 0))
    sq, so = query_weight.shape, output_weight.shape
    return pl.pallas_call(
        finish_kernel,
        grid=(n,),
        out_shape=tuple(
            jax.ShapeDtypeStruct(s, d)
            for s, d in (
                (sq, f32), (so, f32), (sq, f32), (so, f32), (sq, bf), (so, bf),
                (query_moment.shape, f32), (output_moment.shape, f32),
            )
        ),
        in_specs=[
            rows, whole,
            pl.BlockSpec((1, rank, width), lambda i: (0, 0, 0)),
            pl.BlockSpec((1, rank, width // n), lambda i: (1, 0, i)),
            wq, wo,
            pl.BlockSpec((1, share // n, width), lambda i: (0, i, 0)),
            pl.BlockSpec((1, share, width // n), lambda i: (1, 0, i)),
        ],
        out_specs=(wq, wo, wq, wo, wq, wo, mq, mo),
        cost_estimate=pl.CostEstimate(
            flops=4 * depth * rank * width, bytes_accessed=20 * depth * width, transcendentals=0
        ),
    )(query_basis, output_basis, full, full, query_weight, output_weight, mom, mom)


def solution(mesh):
    small = dict(mesh.shape) == {"fs": 4, "rep": 4, "tp": 2}
    body = on_device_fast if small else on_device
    placed = (
        P(("fs", "rep"), None),
        P(("fs", "rep"), "tp"),
        P(("fs", "rep"), "tp"),
        P(("fs", "rep"), None),
        P("fs", None),
        P("fs", None),
        P("fs", "tp"),
        P("tp", "fs"),
        P("rep", "tp"),
        P("tp", "rep"),
    )
    return jax.shard_map(
        body,
        mesh=mesh,
        in_specs=placed,
        out_specs=(
            P("fs", "tp"),
            P("tp", "fs"),
            P("fs", "tp"),
            P("tp", "fs"),
            P("fs", "tp"),
            P("tp", "fs"),
            P("rep", "tp"),
            P("tp", "rep"),
        ),
        check_vma=False,
    )
```
